32 devices in a mesh: ep: 8 (over z, core), tp: 4 (over y, x).
Axes of the slice: x: 2, y: 2, z: 4, core: 2. Of those that a mesh axis runs over, the one named last changes fastest.
Arguments:
- tokens: bfloat16 [4096, 2048], P(('ep', 'tp')), may hold values from -6 to 6
- norm_gain: float32 [2048], replicated, may hold values from 0.1 to 1.9
- expert_ids: int32 [4096, 2], P(('ep', 'tp')), may hold values from 0 to 7, all different within a row; in each aligned block of 128 rows (0 to 127, 128 to 255, ...) at most 64 rows name the same one
- gate_weights: float32 [4096, 2], P(('ep', 'tp')), may hold values from 0.2 to 1.6
- expert_gate: bfloat16 [8, 512, 2048], P('ep', 'tp'), may hold values from -0.125 to 0.125
- expert_up: bfloat16 [8, 512, 2048], P('ep', 'tp'), may hold values from -0.125 to 0.125
- expert_down: bfloat16 [8, 512, 2048], P('ep', 'tp'), may hold values from -0.25 to 0.25
- shared_gate: bfloat16 [512, 2048], P('tp'), may hold values from -0.125 to 0.125
- shared_up: bfloat16 [512, 2048], P('tp'), may hold values from -0.125 to 0.125
- shared_down: bfloat16 [512, 2048], P('tp'), may hold values from -0.25 to 0.25
Outputs:
- mixed: bfloat16 [4096, 2048], P(('ep', 'tp'))
The draws below stay inside these ranges and needn't reach their ends.
Inputs may be any that keep to these rules, and one draw needn't show every extreme that they name: `expert_ids`: each row names 2 different experts. Within the rows of one device no expert is named by more than 64 rows, and in every draw some expert is named by exactly 64 rows of some device.
All inputs are finite; a program needn't handle non-finite values.
Results may differ from the reference program's by a relative error of at most 0.0068.
Values may be sent and summed in bfloat16 or wider, within the bound.
A program may use at most 64 MiB of HBM per device.

```python
import math
import jax
import jax.numpy as jnp
import numpy as np
from jax import lax

D = 2048
FF = 512
SFF = 512
K = 2
TOK_DEV = 128
EXPERTS = 8
CAP = 64
TOKENS = 4096


def block_levels(rng, shape, shards, smallest, largest):
    gain = 1.0
    for dim, parts in shards:
        draws = jax.random.uniform(jax.random.fold_in(jax.random.fold_in(rng, 6), dim), (parts,), jnp.float32, smallest / len(shards), largest / len(shards))
        gain = gain * jnp.repeat(jnp.exp(draws), shape[dim] // parts).reshape((-1,) + (1,) * (len(shape) - 1 - dim))
    return gain


def deal_out(own_key, own, number, rows, amount, top, limit, skew):
    sequence = jax.random.permutation(own_key, amount)
    packed, common = shares(amount, rows * top, limit, skew, True), shares(amount, rows * top, limit, skew, False)
    places = jnp.arange(amount)

    def named(tallies, turn):
        used = int((tallies > 0).sum())
        fixed = max(1, used // 4)
        shifted = fixed + (places - fixed + turn * (used - fixed)) % max(1, amount - fixed)
        return jnp.zeros((amount,), jnp.int32).at[sequence[jnp.where(places < fixed, places, shifted)]].set(jnp.asarray(tallies, jnp.int32))

    tallies = jnp.where(number % 4 == 0, named(packed, number // 4), named(common, number - number // 4 - 1))
    mixed = jax.random.permutation(jax.random.fold_in(own, 3), amount)
    giver, taker = mixed[0:amount // 2 * 2:2], mixed[1:amount // 2 * 2:2]
    slack = jnp.minimum(tallies[giver] - 1, limit - tallies[taker]) // 2
    slack = jnp.where((giver == sequence[0]) | (taker == sequence[0]) | (tallies[taker] == 0), 0, jnp.maximum(slack, 0))
    shifted = jax.random.randint(jax.random.fold_in(own, 4), (amount // 2,), 0, 1 << 20) % (slack + 1)
    tallies = tallies.at[giver].add(-shifted).at[taker].add(shifted)
    members = jnp.searchsorted(jnp.cumsum(tallies), jnp.arange(rows * top), side="right").astype(jnp.int32)
    listing = members.reshape(top, rows).T
    listing = listing[jax.random.permutation(jax.random.fold_in(own, 1), rows)]
    turn = jax.random.randint(jax.random.fold_in(own, 2), (rows, 1), 0, top)
    return jnp.take_along_axis(listing, (jnp.arange(top)[None, :] + turn) % top, axis=1)


def shares(amount, total, bound, lean, full):
    portions = [(1 << 20) // math.isqrt(standing ** lean) + 1 for standing in range(1, amount + 1)]
    largest = bound if full else min(bound, max(-(-total // amount), total * portions[0] // sum(portions)))
    least = 1 if total - largest >= amount - 1 else 0
    counts, rest = [largest] + [least] * (amount - 1), total - largest - least * (amount - 1)
    while rest > 0:
        free = [i for i in range(1, amount) if counts[i] < largest] or [i for i in range(1, amount) if counts[i] < bound]
        mass, left = sum([portions[i] for i in free]), rest
        for i in free:
            addition = min(bound - counts[i], max(1, left * portions[i] // mass), rest)
            counts[i] = counts[i] + addition
            rest = rest - addition
    return np.array(counts)


def normal_values(rng, extent, spread, reach, pieces=(), held_as=jnp.bfloat16):
    values = spread * jax.random.normal(rng, extent, jnp.float32)
    if pieces:
        values = values * block_levels(rng, extent, pieces, -0.22, 0.18)
    return jnp.clip(values, -reach, reach).astype(held_as)


def setup_inputs(seed: int = 0) -> dict:
    seeds = jax.random.split(jax.random.key(seed), 11)
    tokens = normal_values(seeds[0], (TOKENS, D), 1.0, 6.0, ((0, 32),))
    norm_gain = jnp.clip(1.0 + 0.18 * jax.random.normal(seeds[1], (D,), jnp.float32), 0.1, 1.9)
    expert_ids_keys = jax.random.split(jax.random.fold_in(seeds[2], 1), TOKENS // TOK_DEV)
    expert_ids_turns = jax.random.permutation(jax.random.fold_in(seeds[2], 3), TOKENS // TOK_DEV)
    expert_ids = jax.vmap(lambda own, number: deal_out(jax.random.fold_in(seeds[2], 2), own, number, TOK_DEV, EXPERTS, K, CAP, 2))(expert_ids_keys, expert_ids_turns).reshape((TOKENS, K))
    gate_weights = jnp.clip(0.2 + 1.4 * jax.random.uniform(seeds[3], (TOKENS, K), jnp.float32) ** block_levels(seeds[3], (TOKENS, K), ((0, 32),), -0.2, 0.2), 0.2, 1.6)
    expert_gate = normal_values(seeds[4], (EXPERTS, FF, D), D ** -0.5, 0.125, ((0, 8), (1, 4)))
    expert_up = normal_values(seeds[5], (EXPERTS, FF, D), D ** -0.5, 0.125, ((0, 8), (1, 4)))
    expert_down = normal_values(seeds[6], (EXPERTS, FF, D), FF ** -0.5, 0.25, ((0, 8), (1, 4)))
    shared_gate = normal_values(seeds[7], (SFF, D), D ** -0.5, 0.125, ((0, 4),))
    shared_up = normal_values(seeds[8], (SFF, D), D ** -0.5, 0.125, ((0, 4),))
    shared_down = normal_values(seeds[9], (SFF, D), SFF ** -0.5, 0.25, ((0, 4),))
    return {"tokens": tokens, "norm_gain": norm_gain, "expert_ids": expert_ids, "gate_weights": gate_weights, "expert_gate": expert_gate, "expert_up": expert_up, "expert_down": expert_down, "shared_gate": shared_gate, "shared_up": shared_up, "shared_down": shared_down}


EPS = 1e-06

def against(rows, weight):
    return jnp.dot(rows, weight.T, preferred_element_type=jnp.float32)

def reference(tokens, norm_gain, expert_ids, gate_weights, expert_gate, expert_up, expert_down, shared_gate, shared_up, shared_down):
    tok = tokens.astype(jnp.float32)
    normed = (tok * lax.rsqrt(lax.optimization_barrier(jnp.mean(tok * tok, axis=-1, keepdims=True)) + EPS) * norm_gain).astype(jnp.bfloat16)
    most_rows = TOKENS // TOK_DEV * CAP
    order = jnp.arange(TOKENS, dtype=jnp.int32)

    def one_expert(index, routed):
        named = expert_ids == index
        member = jnp.any(named, axis=1).astype(jnp.int32)
        weight_row = lax.optimization_barrier(jnp.sum(jnp.where(named, gate_weights, 0.0), axis=1))
        place = (jnp.cumsum(member) - member).astype(jnp.int32)
        place = jnp.where(member > 0, place, most_rows).astype(jnp.int32)
        table = jnp.full((most_rows,), TOKENS, jnp.int32).at[place].set(order, mode='drop')
        rows = jnp.take(normed, table, axis=0, mode='fill', fill_value=0)
        scale = jnp.take(weight_row, table, axis=0, mode='fill', fill_value=0)
        gate = lax.dynamic_index_in_dim(expert_gate, index, 0, keepdims=False)
        up = lax.dynamic_index_in_dim(expert_up, index, 0, keepdims=False)
        down = lax.dynamic_index_in_dim(expert_down, index, 0, keepdims=False)
        hidden = (jax.nn.silu(against(rows, gate)) * against(rows, up)).astype(jnp.bfloat16)
        result = jnp.dot(hidden, down, preferred_element_type=jnp.float32).astype(jnp.bfloat16)
        return routed.at[table].add(scale[:, None] * result.astype(jnp.float32), mode='drop')
    routed = lax.fori_loop(0, EXPERTS, one_expert, jnp.zeros((TOKENS, D), jnp.float32))
    shared_hidden = (jax.nn.silu(against(normed, shared_gate)) * against(normed, shared_up)).astype(jnp.bfloat16)
    shared = jnp.dot(shared_hidden, shared_down, preferred_element_type=jnp.float32)
    return (routed + shared).astype(jnp.bfloat16)
```

```python
import functools
import math

import jax
import jax.numpy as jnp
from jax import lax
from jax.experimental import pallas as pl
from jax.experimental.pallas import tpu as pltpu
from jax.sharding import PartitionSpec as P

EPS = 1e-06
MESH = pl.DeviceIdType.MESH
NT = (((1,), (1,)), ((), ()))
F32 = jnp.float32
BF16 = jnp.bfloat16


def remote(src, dst, send, recv, where):
    return pltpu.make_async_remote_copy(
        src_ref=src, dst_ref=dst, send_sem=send, recv_sem=recv, device_id=where, device_id_type=MESH
    )


def kernel(
    ep, tp, xs, ys, cap,
    tok_ref, gain_ref, ids_ref, gw_ref, eg, eu, ed, sg, su, sd, out_ref,
    wts, swts, normed, mix, outgoing, arrived, hidden, results, returned,
    s1, r1, s2, r2, s3, r3, sa, ra, sb, rb,
):
    e = lax.axis_index("ep")
    t = lax.axis_index("tp")
    y, x = t // xs, t % xs
    core = e % 2
    partner = e + 1 - 2 * core
    d_model = tok_ref.shape[1]
    rows = tok_ref.shape[0]
    half = d_model // 2
    own_rows = eg.shape[0]
    srows = sg.shape[0] // 2
    slots = ep * cap

    def at(dy, dx):
        return lax.rem(y + dy, ys) * xs + lax.rem(x + dx, xs)

    row_peers = [at(0, i) for i in range(1, xs)]
    col_peers = [at(i, 0) for i in range(1, ys)]
    diagonal = [at(i, j) for i in range(1, ys) for j in range(1, xs)]
    ep_peers = [lax.rem(e + i, ep) for i in range(1, ep)]

    barrier = pltpu.get_barrier_semaphore()
    for p in row_peers + col_peers:
        pl.semaphore_signal(barrier, inc=1, device_id={"tp": p}, device_id_type=MESH)
    for p in ep_peers:
        pl.semaphore_signal(barrier, inc=1, device_id={"ep": p}, device_id_type=MESH)
    pl.semaphore_wait(barrier, len(row_peers) + len(col_peers) + len(ep_peers))

    ins = (eg, eu, ed, sg, su, sd)
    sends = []

    def block(a, owner):
        return wts.at[a, owner] if a < 3 else swts.at[a - 3, core, owner]

    def part(a, owner, h):
        cols = pl.ds(h * half, half)
        return wts.at[a, owner, :, cols] if a < 3 else swts.at[a - 3, core, owner, :, cols]

    def own(a):
        return ins[a] if a < 3 else ins[a].at[pl.ds(pl.multiple_of(core * srows, srows), srows)]

    def first(a):
        for j, p in enumerate(row_peers + col_peers):
            c = remote(own(a), block(a, t), s1.at[a, j], r1.at[a, t], {"tp": p})
            c.start()
            sends.append(c)

    def first_done(a):
        for q in row_peers + col_peers:
            remote(block(a, q), block(a, q), s1.at[a, 0], r1.at[a, q], {"tp": q}).wait_recv()

    def second(a):
        for h, (owners, peers) in enumerate(((col_peers, row_peers), (row_peers, col_peers))):
            for i, q in enumerate(owners):
                for j, p in enumerate(peers):
                    c = remote(part(a, q, h), part(a, q, h), s2.at[a, h, i, j], r2.at[a, h, q], {"tp": p})
                    c.start()
                    sends.append(c)

    def second_done(a):
        for q in diagonal:
            for h in range(2):
                remote(part(a, q, h), part(a, q, h), s2.at[a, h, 0, 0], r2.at[a, h, q], {"tp": q}).wait_recv()

    first(0)
    first(1)

    tok = tok_ref[...].astype(F32)
    nrm = tok * lax.rsqrt(jnp.mean(tok * tok, axis=-1, keepdims=True) + EPS) * gain_ref[...]
    normed[...] = nrm.astype(BF16)
    ids = ids_ref[...]
    chosen = ids.shape[1]
    labels = lax.broadcasted_iota(jnp.int32, (rows, ep), 1)
    one_hot = [(ids[:, k : k + 1] == labels).astype(F32) for k in range(chosen)]
    hits = sum(one_hot[1:], one_hot[0])
    lower = (
        lax.broadcasted_iota(jnp.int32, (rows, rows), 1) < lax.broadcasted_iota(jnp.int32, (rows, rows), 0)
    ).astype(F32).astype(BF16)
    before = jnp.dot(lower, hits.astype(BF16), preferred_element_type=F32)
    slot_ids = lax.broadcasted_iota(jnp.int32, (rows, slots), 1).astype(F32)
    weights = jnp.zeros((rows, slots), F32)
    placing = jnp.zeros((rows, slots), F32)
    for k in range(chosen):
        place = ids[:, k : k + 1].astype(F32) * cap + jnp.sum(before * one_hot[k], axis=1, keepdims=True)
        hit = (place == slot_ids).astype(F32)
        placing = placing + hit
        weights = weights + gw_ref[:, k : k + 1] * hit
    high = weights.astype(BF16)
    mix[0] = high
    mix[1] = (weights - high.astype(F32)).astype(BF16)
    spread = placing.T.astype(BF16)
    for n in range(4):
        cols = slice(n * (d_model // 4), (n + 1) * (d_model // 4))
        o = jnp.dot(spread, normed[:, cols], preferred_element_type=F32).astype(BF16)
        outgoing[:, :, cols] = o.reshape(ep, cap, d_model // 4)

    for j, p in enumerate(ep_peers):
        c = remote(outgoing.at[p], arrived.at[e], sa.at[j], ra.at[e], {"ep": p})
        c.start()
        sends.append(c)
    arrived[e] = outgoing[e]
    for a in range(3):
        wts[a, t] = ins[a][...]
        swts[a, core, t] = ins[a + 3][pl.ds(pl.multiple_of(core * srows, srows), srows), :]

    first_done(0)
    second(0)
    first(2)
    first_done(1)
    second(1)
    first_done(2)
    second(2)
    first(3)
    first(4)

    for p in ep_peers:
        remote(arrived.at[p], arrived.at[p], sa.at[0], ra.at[p], {"ep": p}).wait_recv()
    second_done(0)
    second_done(1)
    per = max(1, min(tp, 256 // own_rows))
    chunks = tp // per
    width = per * own_rows
    for c in range(chunks):
        held = arrived[...].reshape(slots, d_model)
        gate = lax.dot_general(held, wts[0, c * per : (c + 1) * per].reshape(width, d_model), NT, preferred_element_type=F32)
        up = lax.dot_general(held, wts[1, c * per : (c + 1) * per].reshape(width, d_model), NT, preferred_element_type=F32)
        hidden[:, c * width : (c + 1) * width] = (gate * (1.0 / (1.0 + jnp.exp(-gate))) * up).astype(BF16)
    second_done(2)
    for n in range(4):
        cols = slice(n * (d_model // 4), (n + 1) * (d_model // 4))
        down = wts[2, :, :, cols].reshape(tp * own_rows, d_model // 4)
        o = jnp.dot(hidden[...], down, preferred_element_type=F32).astype(BF16)
        results[:, :, cols] = o.reshape(ep, cap, d_model // 4)
    for j, p in enumerate(ep_peers):
        c = remote(results.at[p], returned.at[e], sb.at[j], rb.at[e], {"ep": p})
        c.start()
        sends.append(c)
    returned[e] = results[e]

    first_done(3)
    second(3)
    first(5)
    first_done(4)
    second(4)
    first_done(5)
    second(5)

    def swap(a):
        return remote(swts.at[a, core], swts.at[a, core], s3.at[a], r3.at[a], {"ep": partner})

    for a in range(3):
        second_done(a + 3)
        c = swap(a)
        c.start()
        sends.append(c)
    for a in range(3):
        other = swts.at[a, 1 - core]
        remote(other, other, s3.at[a], r3.at[a], {"ep": partner}).wait_recv()
    sall = swts.shape[1] * tp * srows
    gate = lax.dot_general(normed[...], swts[0].reshape(sall, d_model), NT, preferred_element_type=F32)
    up = lax.dot_general(normed[...], swts[1].reshape(sall, d_model), NT, preferred_element_type=F32)
    shared_hidden = (gate * (1.0 / (1.0 + jnp.exp(-gate))) * up).astype(BF16)

    for p in ep_peers:
        remote(returned.at[p], returned.at[p], sb.at[0], rb.at[p], {"ep": p}).wait_recv()
    for n in range(4):
        cols = slice(n * (d_model // 4), (n + 1) * (d_model // 4))
        sdown = swts[2, :, :, :, cols].reshape(sall, d_model // 4)
        back = returned[:, :, cols].reshape(slots, d_model // 4)
        total = jnp.dot(mix[0], back, preferred_element_type=F32)
        total = total + jnp.dot(mix[1], back, preferred_element_type=F32)
        total = total + jnp.dot(shared_hidden, sdown, preferred_element_type=F32)
        out_ref[:, cols] = total.astype(BF16)
    for c in sends:
        c.wait_send()


def body(ep, tp, tokens, norm_gain, expert_ids, gate_weights, eg, eu, ed, sg, su, sd):
    rows, d_model = tokens.shape
    cap = 2 * rows * expert_ids.shape[1] // ep
    side = math.isqrt(tp)
    xs = side if side * side == tp else tp
    ys = tp // xs
    own_rows = eg.shape[1]
    srows = sg.shape[0] // 2
    near = xs + ys - 2
    far = max(xs, ys)
    dma = pltpu.SemaphoreType.DMA
    vm = pl.BlockSpec(memory_space=pltpu.VMEM)
    return pl.pallas_call(
        functools.partial(kernel, ep, tp, xs, ys, cap),
        out_shape=jax.ShapeDtypeStruct((rows, d_model), BF16),
        in_specs=[vm] * 10,
        out_specs=vm,
        scratch_shapes=[
            pltpu.VMEM((3, tp, own_rows, d_model), BF16),
            pltpu.VMEM((3, 2, tp, srows, d_model), BF16),
            pltpu.VMEM((rows, d_model), BF16),
            pltpu.VMEM((2, rows, ep * cap), BF16),
            pltpu.VMEM((ep, cap, d_model), BF16),
            pltpu.VMEM((ep, cap, d_model), BF16),
            pltpu.VMEM((ep * cap, tp * own_rows), BF16),
            pltpu.VMEM((ep, cap, d_model), BF16),
            pltpu.VMEM((ep, cap, d_model), BF16),
            dma((6, near)),
            dma((6, tp)),
            dma((6, 2, far, far)),
            dma((6, 2, tp)),
            dma((3,)),
            dma((3,)),
            dma((ep,)),
            dma((ep,)),
            dma((ep,)),
            dma((ep,)),
        ],
        compiler_params=pltpu.CompilerParams(
            collective_id=0, has_side_effects=True, vmem_limit_bytes=62 * 1024 * 1024
        ),
        name="moe",
    )(tokens, norm_gain.reshape(1, d_model), expert_ids, gate_weights, eg[0], eu[0], ed[0], sg, su, sd)


def solution(mesh):
    in_specs = (
        P(("ep", "tp"), None),
        P(),
        P(("ep", "tp"), None),
        P(("ep", "tp"), None),
        P("ep", "tp", None),
        P("ep", "tp", None),
        P("ep", "tp", None),
        P("tp", None),
        P("tp", None),
        P("tp", None),
    )
    out_specs = P(("ep", "tp"), None)
    return jax.shard_map(
        functools.partial(body, mesh.shape["ep"], mesh.shape["tp"]),
        mesh=mesh, in_specs=in_specs, out_specs=out_specs, check_vma=False,
    )
```

```python
import functools
import math

import jax
import jax.numpy as jnp
from jax import lax
from jax.experimental import pallas as pl
from jax.experimental.pallas import tpu as pltpu
from jax.sharding import PartitionSpec as P

EPS = 1e-06
MESH = pl.DeviceIdType.MESH
NT = (((1,), (1,)), ((), ()))
F32 = jnp.float32
BF16 = jnp.bfloat16
CHUNKS = 4


def remote(src, dst, send, recv, where):
    return pltpu.make_async_remote_copy(
        src_ref=src, dst_ref=dst, send_sem=send, recv_sem=recv, device_id=where, device_id_type=MESH
    )


def kernel(
    ep, tp, xs, ys, cap,
    tok_ref, gain_ref, ids_ref, gw_ref, eg, eu, ed, sg, su, sd, out_ref,
    wts, swts, normed, mix, spread, pick, tokens, arrived, hidden, results, returned,
    s1, r1, s2, r2, s3, r3, sp, rp, st, rt, sd2, rd2, sb, rb,
):
    e = lax.axis_index("ep")
    t = lax.axis_index("tp")
    y, x = t // xs, t % xs
    z, core = e // 2, e % 2
    nz = ep // 2
    partner = e + 1 - 2 * core
    rows, d_model = tok_ref.shape
    own_rows = eg.shape[0]
    srows = sg.shape[0] // 2
    slots = ep * cap
    piece = d_model // CHUNKS
    last = 2 + CHUNKS

    def at(dy, dx):
        return lax.rem(y + dy, ys) * xs + lax.rem(x + dx, xs)

    row_peers = [at(0, i) for i in range(1, xs)]
    col_peers = [at(i, 0) for i in range(1, ys)]
    diagonal = [at(i, j) for i in range(1, ys) for j in range(1, xs)]
    ep_peers = [lax.rem(e + i, ep) for i in range(1, ep)]

    barrier = pltpu.get_barrier_semaphore()
    for p in row_peers + col_peers:
        pl.semaphore_signal(barrier, inc=1, device_id={"tp": p}, device_id_type=MESH)
    for p in ep_peers:
        pl.semaphore_signal(barrier, inc=1, device_id={"ep": p}, device_id_type=MESH)
    pl.semaphore_wait(barrier, len(row_peers) + len(col_peers) + len(ep_peers))

    sends = []
    mine = pl.ds(pl.multiple_of(core * srows, srows), srows)

    def columns(a):
        return ((a - 2) * piece, piece) if 2 <= a < last else (0, d_model)

    def view(a, owner, start, size):
        cols = pl.ds(start, size)
        if a < last:
            return wts.at[min(a, 2), owner, :, cols]
        return swts.at[a - last, core, owner, :, cols]

    def block(a, owner):
        return view(a, owner, *columns(a))

    def part(a, owner, h):
        start, size = columns(a)
        return view(a, owner, start + h * (size // 2), size // 2)

    def own(a):
        if a < last:
            start, size = columns(a)
            return (eg, eu, ed)[min(a, 2)].at[:, pl.ds(start, size)]
        return (sg, su, sd)[a - last].at[mine]

    def first(a):
        for j, p in enumerate(row_peers + col_peers):
            c = remote(own(a), block(a, t), s1.at[a, j], r1.at[a, t], {"tp": p})
            c.start()
            sends.append(c)

    def first_done(a):
        for q in row_peers + col_peers:
            remote(block(a, q), block(a, q), s1.at[a, 0], r1.at[a, q], {"tp": q}).wait_recv()

    def second(a):
        for h, (owners, peers) in enumerate(((col_peers, row_peers), (row_peers, col_peers))):
            for i, q in enumerate(owners):
                for j, p in enumerate(peers):
                    c = remote(part(a, q, h), part(a, q, h), s2.at[a, h, i, j], r2.at[a, h, q], {"tp": p})
                    c.start()
                    sends.append(c)

    def second_done(a):
        for q in diagonal:
            for h in range(2):
                remote(part(a, q, h), part(a, q, h), s2.at[a, h, 0, 0], r2.at[a, h, q], {"tp": q}).wait_recv()

    def hop(src, sign, source):
        slot = 2 * src + core
        d = 0 if sign > 0 else 1
        return remote(source, tokens.at[slot], st.at[d, src], rt.at[src], {"ep": e + 2 * sign})

    def over(src, source):
        slot = 2 * src + core
        return remote(source, tokens.at[slot], sd2.at[src], rd2.at[src], {"ep": partner})

    def from_partner(src):
        slot = 2 * src + 1 - core
        return remote(tokens.at[slot], tokens.at[slot], sd2.at[src], rd2.at[src], {"ep": partner})

    def pack(src_ep, source):
        raw = jnp.dot(pick[src_ep], source[...], preferred_element_type=F32)
        scale = lax.rsqrt(jnp.mean(raw * raw, axis=-1, keepdims=True) + EPS)
        arrived[src_ep] = (raw * scale * gain_ref[...]).astype(BF16)

    def pick_done(src_ep):
        remote(pick.at[src_ep], pick.at[src_ep], sp.at[0], rp.at[src_ep], {"ep": partner}).wait_recv()

    first(0)

    @pl.when(z + 1 < nz)
    def _():
        hop(z, 1, tok_ref).start()

    @pl.when(z > 0)
    def _():
        hop(z, -1, tok_ref).start()

    over(z, tok_ref).start()
    first(1)

    ids = ids_ref[...]
    chosen = ids.shape[1]
    labels = lax.broadcasted_iota(jnp.int32, (rows, ep), 1)
    one_hot = [(ids[:, k : k + 1] == labels).astype(F32) for k in range(chosen)]
    hits = sum(one_hot[1:], one_hot[0])
    lower = (
        lax.broadcasted_iota(jnp.int32, (rows, rows), 1) < lax.broadcasted_iota(jnp.int32, (rows, rows), 0)
    ).astype(F32).astype(BF16)
    before = jnp.dot(lower, hits.astype(BF16), preferred_element_type=F32)
    slot_ids = lax.broadcasted_iota(jnp.int32, (rows, slots), 1).astype(F32)
    weights = jnp.zeros((rows, slots), F32)
    placing = jnp.zeros((rows, slots), F32)
    for k in range(chosen):
        place = ids[:, k : k + 1].astype(F32) * cap + jnp.sum(before * one_hot[k], axis=1, keepdims=True)
        hit = (place == slot_ids).astype(F32)
        placing = placing + hit
        weights = weights + gw_ref[:, k : k + 1] * hit
    spread[...] = placing.T.astype(BF16).reshape(ep, cap, rows)
    high = weights.astype(BF16)
    mix[0] = high
    mix[1] = (weights - high.astype(F32)).astype(BF16)
    for j, p in enumerate(ep_peers):
        c = remote(spread.at[p], pick.at[e], sp.at[j], rp.at[e], {"ep": p})
        c.start()
        sends.append(c)
    pick[e] = spread[e]
    tok = tok_ref[...].astype(F32)
    nrm = tok * lax.rsqrt(jnp.mean(tok * tok, axis=-1, keepdims=True) + EPS) * gain_ref[...]
    normed[...] = nrm.astype(BF16)
    for a, ref in enumerate((eg, eu, ed)):
        wts[a, t] = ref[...]
    for a, ref in enumerate((sg, su, sd)):
        swts[a, core, t] = ref[mine, :]
    pack(e, tok_ref)
    for p in ep_peers:
        pick_done(p)
    from_partner(z).wait_recv()
    pack(partner, tokens.at[partner])

    first_done(0)
    second(0)

    def packs(step):
        for sign in (1, -1):
            src = z - sign * (step + 1)
            there = (src >= 0) if sign > 0 else (src < nz)

            @pl.when(there)
            def _():
                pack(2 * src + core, tokens.at[2 * src + core])
                from_partner(src).wait_recv()
                pack(2 * src + 1 - core, tokens.at[2 * src + 1 - core])

    for step in range(nz - 1):
        for sign in (1, -1):
            src = z - sign * (step + 1)
            there = (src >= 0) if sign > 0 else (src < nz)
            on = (z + 1 < nz) if sign > 0 else (z > 0)

            @pl.when(there)
            def _():
                here = tokens.at[2 * src + core]
                hop(src, sign, here).wait_recv()

                @pl.when(on)
                def _():
                    hop(src, sign, here).start()

                over(src, here).start()

        if step == 0:
            packs(0)
            first_done(1)
            second(1)
            first(2)
            first(3)
        else:
            packs(step)
    if nz == 1:
        first_done(1)
        second(1)
        first(2)
        first(3)

    second_done(0)
    second_done(1)
    per = max(1, min(tp, 256 // own_rows))
    width = per * own_rows
    for c in range(tp // per):
        held = arrived[...].reshape(slots, d_model)
        gate = lax.dot_general(held, wts[0, c * per : (c + 1) * per].reshape(width, d_model), NT, preferred_element_type=F32)
        up = lax.dot_general(held, wts[1, c * per : (c + 1) * per].reshape(width, d_model), NT, preferred_element_type=F32)
        hidden[:, c * width : (c + 1) * width] = (gate * (1.0 / (1.0 + jnp.exp(-gate))) * up).astype(BF16)

    def back(n, p, j):
        cols = pl.ds(n * piece, piece)
        return remote(results.at[p, :, cols], returned.at[e, :, cols], sb.at[n, j], rb.at[n, e], {"ep": p})

    total = last + 3
    for n in range(CHUNKS):
        a = n + 2
        if n == 0:
            first_done(a)
            second(a)
            first(a + 2)
        first_done(a + 1)
        second(a + 1)
        if a + 3 < total:
            first(a + 3)
        second_done(a)
        cols = slice(n * piece, (n + 1) * piece)
        down = wts[2, :, :, cols].reshape(tp * own_rows, piece)
        o = jnp.dot(hidden[...], down, preferred_element_type=F32).astype(BF16)
        results[:, :, cols] = o.reshape(ep, cap, piece)
        for j, p in enumerate(ep_peers):
            c = back(n, p, j)
            c.start()
            sends.append(c)
        returned[e, :, cols] = results[e, :, cols]

    def swap(a):
        return remote(swts.at[a, core], swts.at[a, core], s3.at[a], r3.at[a], {"ep": partner})

    for a in range(3):
        if a > 0:
            first_done(last + a)
            second(last + a)
        second_done(last + a)
        c = swap(a)
        c.start()
        sends.append(c)
    for a in range(3):
        other = swts.at[a, 1 - core]
        remote(other, other, s3.at[a], r3.at[a], {"ep": partner}).wait_recv()
    sall = 2 * tp * srows
    gate = lax.dot_general(normed[...], swts[0].reshape(sall, d_model), NT, preferred_element_type=F32)
    up = lax.dot_general(normed[...], swts[1].reshape(sall, d_model), NT, preferred_element_type=F32)
    shared_hidden = (gate * (1.0 / (1.0 + jnp.exp(-gate))) * up).astype(BF16)

    for n in range(CHUNKS):
        cols = slice(n * piece, (n + 1) * piece)
        sdown = swts[2, :, :, :, cols].reshape(sall, piece)
        sum_shared = jnp.dot(shared_hidden, sdown, preferred_element_type=F32)
        for p in ep_peers:
            c = returned.at[p, :, pl.ds(n * piece, piece)]
            remote(c, c, sb.at[0, 0], rb.at[n, p], {"ep": p}).wait_recv()
        given = returned[:, :, cols].reshape(slots, piece)
        routed = jnp.dot(mix[0], given, preferred_element_type=F32)
        routed = routed + jnp.dot(mix[1], given, preferred_element_type=F32)
        out_ref[:, cols] = (routed + sum_shared).astype(BF16)
    for c in sends:
        c.wait_send()

    over(z, tok_ref).wait_send()

    @pl.when(z + 1 < nz)
    def _():
        hop(z, 1, tok_ref).wait_send()

    @pl.when(z > 0)
    def _():
        hop(z, -1, tok_ref).wait_send()

    for step in range(nz - 1):
        for sign in (1, -1):
            src = z - sign * (step + 1)
            there = (src >= 0) if sign > 0 else (src < nz)
            on = (z + 1 < nz) if sign > 0 else (z > 0)

            @pl.when(there)
            def _():
                here = tokens.at[2 * src + core]
                over(src, here).wait_send()

                @pl.when(on)
                def _():
                    hop(src, sign, here).wait_send()


def body(ep, tp, tokens, norm_gain, expert_ids, gate_weights, eg, eu, ed, sg, su, sd):
    rows, d_model = tokens.shape
    cap = 2 * rows * expert_ids.shape[1] // ep
    side = math.isqrt(tp)
    xs = side if side * side == tp else tp
    ys = tp // xs
    own_rows = eg.shape[1]
    srows = sg.shape[0] // 2
    near = xs + ys - 2
    far = max(xs, ys)
    moves = 2 + CHUNKS + 3
    dma = pltpu.SemaphoreType.DMA
    vm = pl.BlockSpec(memory_space=pltpu.VMEM)
    return pl.pallas_call(
        functools.partial(kernel, ep, tp, xs, ys, cap),
        out_shape=jax.ShapeDtypeStruct((rows, d_model), BF16),
        in_specs=[vm] * 10,
        out_specs=vm,
        scratch_shapes=[
            pltpu.VMEM((3, tp, own_rows, d_model), BF16),
            pltpu.VMEM((3, 2, tp, srows, d_model), BF16),
            pltpu.VMEM((rows, d_model), BF16),
            pltpu.VMEM((2, rows, ep * cap), BF16),
            pltpu.VMEM((ep, cap, rows), BF16),
            pltpu.VMEM((ep, cap, rows), BF16),
            pltpu.VMEM((ep, rows, d_model), BF16),
            pltpu.VMEM((ep, cap, d_model), BF16),
            pltpu.VMEM((ep * cap, tp * own_rows), BF16),
            pltpu.VMEM((ep, cap, d_model), BF16),
            pltpu.VMEM((ep, cap, d_model), BF16),
            dma((moves, near)),
            dma((moves, tp)),
            dma((moves, 2, far, far)),
            dma((moves, 2, tp)),
            dma((3,)),
            dma((3,)),
            dma((ep,)),
            dma((ep,)),
            dma((2, ep // 2)),
            dma((ep // 2,)),
            dma((ep // 2,)),
            dma((ep // 2,)),
            dma((CHUNKS, ep)),
            dma((CHUNKS, ep)),
        ],
        compiler_params=pltpu.CompilerParams(
            collective_id=0, has_side_effects=True, vmem_limit_bytes=62 * 1024 * 1024
        ),
        name="moe",
    )(tokens, norm_gain.reshape(1, d_model), expert_ids, gate_weights, eg[0], eu[0], ed[0], sg, su, sd)


def solution(mesh):
    in_specs = (
        P(("ep", "tp"), None),
        P(),
        P(("ep", "tp"), None),
        P(("ep", "tp"), None),
        P("ep", "tp", None),
        P("ep", "tp", None),
        P("ep", "tp", None),
        P("tp", None),
        P("tp", None),
        P("tp", None),
    )
    out_specs = P(("ep", "tp"), None)
    return jax.shard_map(
        functools.partial(body, mesh.shape["ep"], mesh.shape["tp"]),
        mesh=mesh, in_specs=in_specs, out_specs=out_specs, check_vma=False,
    )
```

```python
import functools
import math

import jax
import jax.numpy as jnp
from jax import lax
from jax.experimental import pallas as pl
from jax.experimental.pallas import tpu as pltpu
from jax.sharding import PartitionSpec as P

EPS = 1e-06
MESH = pl.DeviceIdType.MESH
NT = (((1,), (1,)), ((), ()))
F32 = jnp.float32
BF16 = jnp.bfloat16
CHUNKS = 4


def remote(src, dst, send, recv, where):
    return pltpu.make_async_remote_copy(
        src_ref=src, dst_ref=dst, send_sem=send, recv_sem=recv, device_id=where, device_id_type=MESH
    )


def kernel(
    ep, tp, xs, ys, cap,
    tok_ref, gain_ref, route_ref, eg, eu, ed, sg, su, sd, out_ref,
    wts, swts, normed, mix, spread, pick, tokens, arrived, hidden, results, returned,
    s1, r1, s2, r2, s3, r3, sp, rp, st, rt, sd2, rd2, sb, rb,
):
    e = lax.axis_index("ep")
    t = lax.axis_index("tp")
    y, x = t // xs, t % xs
    z, core = e // 2, e % 2
    nz = ep // 2
    partner = e + 1 - 2 * core
    rows, d_model = tok_ref.shape
    own_rows = eg.shape[0]
    srows = sg.shape[0] // 2
    slots = ep * cap
    piece = d_model // CHUNKS
    last = 2 + CHUNKS

    def at(dy, dx):
        return lax.rem(y + dy, ys) * xs + lax.rem(x + dx, xs)

    row_peers = [at(0, i) for i in range(1, xs)]
    col_peers = [at(i, 0) for i in range(1, ys)]
    diagonal = [at(i, j) for i in range(1, ys) for j in range(1, xs)]
    if ep & (ep - 1) == 0:
        bits = [1 << b for b in range(ep.bit_length() - 1)]
        ep_peers = [sum((e // b + i // b) % 2 * b for b in bits) for i in range(ep - 1, 0, -1)]
    else:
        ep_peers = [lax.rem(e + i, ep) for i in range(1, ep)]

    barrier = pltpu.get_barrier_semaphore()
    for p in row_peers + col_peers:
        pl.semaphore_signal(barrier, inc=1, device_id={"tp": p}, device_id_type=MESH)
    for p in ep_peers:
        pl.semaphore_signal(barrier, inc=1, device_id={"ep": p}, device_id_type=MESH)
    pl.semaphore_wait(barrier, len(row_peers) + len(col_peers) + len(ep_peers))

    sends = []
    mine = pl.ds(pl.multiple_of(core * srows, srows), srows)

    def columns(a):
        return ((a - 2) * piece, piece) if 2 <= a < last else (0, d_model)

    def view(a, owner, start, size):
        cols = pl.ds(start, size)
        if a < last:
            return wts.at[min(a, 2), owner, :, cols]
        return swts.at[a - last, core, owner, :, cols]

    def block(a, owner):
        return view(a, owner, *columns(a))

    def part(a, owner, h):
        start, size = columns(a)
        return view(a, owner, start + h * (size // 2), size // 2)

    def own(a):
        if a < last:
            start, size = columns(a)
            return (eg, eu, ed)[min(a, 2)].at[:, pl.ds(start, size)]
        return (sg, su, sd)[a - last].at[mine]

    def first(a):
        for j, p in enumerate(row_peers + col_peers):
            c = remote(own(a), block(a, t), s1.at[a, j], r1.at[a, t], {"tp": p})
            c.start()
            sends.append(c)

    def first_done(a):
        for q in row_peers + col_peers:
            remote(block(a, q), block(a, q), s1.at[a, 0], r1.at[a, q], {"tp": q}).wait_recv()

    def second(a):
        for h, (owners, peers) in enumerate(((col_peers, row_peers), (row_peers, col_peers))):
            for i, q in enumerate(owners):
                for j, p in enumerate(peers):
                    c = remote(part(a, q, h), part(a, q, h), s2.at[a, h, i, j], r2.at[a, h, q], {"tp": p})
                    c.start()
                    sends.append(c)

    def second_done(a):
        for q in diagonal:
            for h in range(2):
                remote(part(a, q, h), part(a, q, h), s2.at[a, h, 0, 0], r2.at[a, h, q], {"tp": q}).wait_recv()

    def hop(src, sign, source):
        slot = 2 * src + core
        d = 0 if sign > 0 else 1
        return remote(source, tokens.at[slot], st.at[d, src], rt.at[src], {"ep": e + 2 * sign})

    def over(src, source):
        slot = 2 * src + core
        return remote(source, tokens.at[slot], sd2.at[src], rd2.at[src], {"ep": partner})

    def from_partner(src):
        slot = 2 * src + 1 - core
        return remote(tokens.at[slot], tokens.at[slot], sd2.at[src], rd2.at[src], {"ep": partner})

    def pack(src_ep, source):
        raw = jnp.dot(pick[src_ep], source[...], preferred_element_type=F32)
        scale = lax.rsqrt(jnp.mean(raw * raw, axis=-1, keepdims=True) + EPS)
        arrived[src_ep] = (raw * scale * gain_ref[...]).astype(BF16)

    def pick_done(src_ep):
        remote(pick.at[src_ep], pick.at[src_ep], sp.at[0], rp.at[src_ep], {"ep": partner}).wait_recv()

    first(0)

    @pl.when(z + 1 < nz)
    def _():
        hop(z, 1, tok_ref).start()

    @pl.when(z > 0)
    def _():
        hop(z, -1, tok_ref).start()

    over(z, tok_ref).start()
    first(1)

    chosen = route_ref.shape[1] // 2
    ids = route_ref[:, :chosen]
    labels = lax.broadcasted_iota(jnp.int32, (rows, ep), 1).astype(F32)
    one_hot = [(ids[:, k : k + 1] == labels).astype(F32) for k in range(chosen)]
    hits = sum(one_hot[1:], one_hot[0])
    lower = (
        lax.broadcasted_iota(jnp.int32, (rows, rows), 1) < lax.broadcasted_iota(jnp.int32, (rows, rows), 0)
    ).astype(F32).astype(BF16)
    before = jnp.dot(lower, hits.astype(BF16), preferred_element_type=F32)
    slot_ids = lax.broadcasted_iota(jnp.int32, (rows, slots), 1).astype(F32)
    weights = jnp.zeros((rows, slots), F32)
    placing = jnp.zeros((rows, slots), F32)
    for k in range(chosen):
        place = ids[:, k : k + 1] * cap + jnp.sum(before * one_hot[k], axis=1, keepdims=True)
        hit = (place == slot_ids).astype(F32)
        placing = placing + hit
        weights = weights + route_ref[:, chosen + k : chosen + k + 1] * hit
    spread[...] = placing.T.astype(BF16).reshape(ep, cap, rows)
    high = weights.astype(BF16)
    mix[0] = high
    mix[1] = (weights - high.astype(F32)).astype(BF16)
    for j, p in enumerate(ep_peers):
        c = remote(spread.at[p], pick.at[e], sp.at[j], rp.at[e], {"ep": p})
        c.start()
        sends.append(c)
    pick[e] = spread[e]
    tok = tok_ref[...].astype(F32)
    nrm = tok * lax.rsqrt(jnp.mean(tok * tok, axis=-1, keepdims=True) + EPS) * gain_ref[...]
    normed[...] = nrm.astype(BF16)
    for a, ref in enumerate((eg, eu, ed)):
        wts[a, t] = ref[...]
    for a, ref in enumerate((sg, su, sd)):
        swts[a, core, t] = ref[mine, :]
    pack(e, tok_ref)
    for p in ep_peers:
        pick_done(p)
    from_partner(z).wait_recv()
    pack(partner, tokens.at[partner])

    first_done(0)
    second(0)

    def packs(step):
        for sign in (1, -1):
            src = z - sign * (step + 1)
            there = (src >= 0) if sign > 0 else (src < nz)

            @pl.when(there)
            def _():
                pack(2 * src + core, tokens.at[2 * src + core])
                from_partner(src).wait_recv()
                pack(2 * src + 1 - core, tokens.at[2 * src + 1 - core])

    for step in range(nz - 1):
        for sign in (1, -1):
            src = z - sign * (step + 1)
            there = (src >= 0) if sign > 0 else (src < nz)
            on = (z + 1 < nz) if sign > 0 else (z > 0)

            @pl.when(there)
            def _():
                here = tokens.at[2 * src + core]
                hop(src, sign, here).wait_recv()

                @pl.when(on)
                def _():
                    hop(src, sign, here).start()

                over(src, here).start()

        if step == 0:
            packs(0)
            first_done(1)
            second(1)
            first(2)
        else:
            packs(step)
    if nz == 1:
        first_done(1)
        second(1)
        first(2)

    first_done(2)
    second(2)
    first(3)
    first(4)
    second_done(0)
    second_done(1)
    per = max(1, min(tp, 256 // own_rows))
    width = per * own_rows
    for c in range(tp // per):
        held = arrived[...].reshape(slots, d_model)
        gate = lax.dot_general(held, wts[0, c * per : (c + 1) * per].reshape(width, d_model), NT, preferred_element_type=F32)
        up = lax.dot_general(held, wts[1, c * per : (c + 1) * per].reshape(width, d_model), NT, preferred_element_type=F32)
        hidden[:, c * width : (c + 1) * width] = (gate * (1.0 / (1.0 + jnp.exp(-gate))) * up).astype(BF16)

    def back(n, p, j):
        cols = pl.ds(n * piece, piece)
        return remote(results.at[p, :, cols], returned.at[e, :, cols], sb.at[n, j], rb.at[n, e], {"ep": p})

    total = last + 3
    for n in range(CHUNKS):
        second_done(n + 2)
        cols = slice(n * piece, (n + 1) * piece)
        down = wts[2, :, :, cols].reshape(tp * own_rows, piece)
        o = jnp.dot(hidden[...], down, preferred_element_type=F32).astype(BF16)
        results[:, :, cols] = o.reshape(ep, cap, piece)
        for j, p in enumerate(ep_peers):
            c = back(n, p, j)
            c.start()
            sends.append(c)
        returned[e, :, cols] = results[e, :, cols]
        first_done(n + 3)
        second(n + 3)
        if n + 5 < total:
            first(n + 5)

    def swap(a):
        return remote(swts.at[a, core], swts.at[a, core], s3.at[a], r3.at[a], {"ep": partner})

    for a in range(1, 3):
        first_done(last + a)
        second(last + a)
    for a in range(3):
        second_done(last + a)
        c = swap(a)
        c.start()
        sends.append(c)
    for a in range(3):
        other = swts.at[a, 1 - core]
        remote(other, other, s3.at[a], r3.at[a], {"ep": partner}).wait_recv()
    sall = 2 * tp * srows
    gate = lax.dot_general(normed[...], swts[0].reshape(sall, d_model), NT, preferred_element_type=F32)
    up = lax.dot_general(normed[...], swts[1].reshape(sall, d_model), NT, preferred_element_type=F32)
    shared_hidden = (gate * (1.0 / (1.0 + jnp.exp(-gate))) * up).astype(BF16)

    for n in range(CHUNKS):
        cols = slice(n * piece, (n + 1) * piece)
        sdown = swts[2, :, :, :, cols].reshape(sall, piece)
        sum_shared = jnp.dot(shared_hidden, sdown, preferred_element_type=F32)
        for p in ep_peers:
            c = returned.at[p, :, pl.ds(n * piece, piece)]
            remote(c, c, sb.at[0, 0], rb.at[n, p], {"ep": p}).wait_recv()
        given = returned[:, :, cols].reshape(slots, piece)
        routed = jnp.dot(mix[0], given, preferred_element_type=F32)
        routed = routed + jnp.dot(mix[1], given, preferred_element_type=F32)
        out_ref[:, cols] = (routed + sum_shared).astype(BF16)
    for c in sends:
        c.wait_send()

    over(z, tok_ref).wait_send()

    @pl.when(z + 1 < nz)
    def _():
        hop(z, 1, tok_ref).wait_send()

    @pl.when(z > 0)
    def _():
        hop(z, -1, tok_ref).wait_send()

    for step in range(nz - 1):
        for sign in (1, -1):
            src = z - sign * (step + 1)
            there = (src >= 0) if sign > 0 else (src < nz)
            on = (z + 1 < nz) if sign > 0 else (z > 0)

            @pl.when(there)
            def _():
                here = tokens.at[2 * src + core]
                over(src, here).wait_send()

                @pl.when(on)
                def _():
                    hop(src, sign, here).wait_send()


def body(ep, tp, tokens, norm_gain, expert_ids, gate_weights, eg, eu, ed, sg, su, sd):
    rows, d_model = tokens.shape
    cap = 2 * rows * expert_ids.shape[1] // ep
    side = math.isqrt(tp)
    xs = side if side * side == tp else tp
    ys = tp // xs
    own_rows = eg.shape[1]
    srows = sg.shape[0] // 2
    near = xs + ys - 2
    route = jnp.concatenate([expert_ids.astype(F32), gate_weights], axis=1)
    far = max(xs, ys)
    moves = 2 + CHUNKS + 3
    dma = pltpu.SemaphoreType.DMA
    vm = pl.BlockSpec(memory_space=pltpu.VMEM)
    return pl.pallas_call(
        functools.partial(kernel, ep, tp, xs, ys, cap),
        out_shape=jax.ShapeDtypeStruct((rows, d_model), BF16),
        in_specs=[vm] * 9,
        out_specs=vm,
        scratch_shapes=[
            pltpu.VMEM((3, tp, own_rows, d_model), BF16),
            pltpu.VMEM((3, 2, tp, srows, d_model), BF16),
            pltpu.VMEM((rows, d_model), BF16),
            pltpu.VMEM((2, rows, ep * cap), BF16),
            pltpu.VMEM((ep, cap, rows), BF16),
            pltpu.VMEM((ep, cap, rows), BF16),
            pltpu.VMEM((ep, rows, d_model), BF16),
            pltpu.VMEM((ep, cap, d_model), BF16),
            pltpu.VMEM((ep * cap, tp * own_rows), BF16),
            pltpu.VMEM((ep, cap, d_model), BF16),
            pltpu.VMEM((ep, cap, d_model), BF16),
            dma((moves, near)),
            dma((moves, tp)),
            dma((moves, 2, far, far)),
            dma((moves, 2, tp)),
            dma((3,)),
            dma((3,)),
            dma((ep,)),
            dma((ep,)),
            dma((2, ep // 2)),
            dma((ep // 2,)),
            dma((ep // 2,)),
            dma((ep // 2,)),
            dma((CHUNKS, ep)),
            dma((CHUNKS, ep)),
        ],
        compiler_params=pltpu.CompilerParams(
            collective_id=0, has_side_effects=True, vmem_limit_bytes=62 * 1024 * 1024
        ),
        name="moe",
    )(tokens, norm_gain.reshape(1, d_model), route, eg[0], eu[0], ed[0], sg, su, sd)


def solution(mesh):
    in_specs = (
        P(("ep", "tp"), None),
        P(),
        P(("ep", "tp"), None),
        P(("ep", "tp"), None),
        P("ep", "tp", None),
        P("ep", "tp", None),
        P("ep", "tp", None),
        P("tp", None),
        P("tp", None),
        P("tp", None),
    )
    out_specs = P(("ep", "tp"), None)
    return jax.shard_map(
        functools.partial(body, mesh.shape["ep"], mesh.shape["tp"]),
        mesh=mesh, in_specs=in_specs, out_specs=out_specs, check_vma=False,
    )
```
